1024 devices in a mesh: kv: 256 (over z, y, core), tp: 4 (over x).
Axes of the slice: x: 4, y: 8, z: 16, core: 2. Of those that a mesh axis runs over, the one named last changes fastest.
Arguments:
- hidden_rows: bfloat16 [98304, 2048], P('kv'), may hold values from -6 to 6
- proj_query: bfloat16 [2048, 2048], P(None, 'tp'), may hold values from -0.125 to 0.125
- proj_key: bfloat16 [2048, 256], P(None, 'tp'), may hold values from -0.125 to 0.125
- proj_value: bfloat16 [2048, 256], P(None, 'tp'), may hold values from -0.125 to 0.125
- proj_output: bfloat16 [2048, 2048], P('tp'), may hold values from -0.125 to 0.125
- head_scale: float32 [32], P('tp'), may hold values from 0.25 to 96
- hot_blocks: int32 [16], replicated, may hold values from 0 to 3071, as said below
- chosen_blocks: int32 [1536, 16], P('kv'), may hold values from 0 to 27, as said below
Outputs:
- layer_out: bfloat16 [98304, 2048], P('kv', 'tp')
The draws below stay inside these ranges and needn't reach their ends.
Inputs may be any that keep to these rules, and one draw needn't show every extreme that they name: `hot_blocks`: 16 different key-block numbers; no device's 12 key blocks hold more than 2 of them, and in every draw some device holds exactly 2. `chosen_blocks`: each row's 16 codes name different key blocks; among them are the key blocks that cover the positions of query block b; no code of 12 or more names a block on the query block's own device.
All inputs are finite; a program needn't handle non-finite values.
Results may differ from the reference program's by a relative error of at most 0.01.
The reference program's roundings to bfloat16 on the way count: a program that leaves them out, or rounds other values in their place, can miss the bound.
Values may be sent and summed in bfloat16 or wider, within the bound.
A program may use at most 32 MiB of HBM per device.

```python
import math
import jax
import jax.numpy as jnp
from jax import lax

D = 2048
H = 32
HD = 64
KVH = 4
KB = 32
QB = 64
NSEL = 16
NHOT = 16
TOK_DEV = 384
SEQ = 98304
NQB = 1536
NKB = 3072
KB_DEV = 12
N_KV = 256
N_TP = 4


def make_hot(key):
    base = jax.random.fold_in(key, 7001)
    key_perm, key_block, key_step, key_order = jax.random.split(base, 4)
    owners = jax.random.permutation(key_perm, N_KV).astype(jnp.int32)
    leader = owners[0]
    opposite = (leader + N_KV // 2) % N_KV
    remaining = owners[1:]
    order = jnp.argsort((remaining == opposite).astype(jnp.int32), stable=True)
    others = remaining[order][:NHOT - 3]
    owner_list = jnp.concatenate([jnp.stack([leader, leader, opposite]), others])
    blocks = jax.random.randint(key_block, (NHOT,), 0, KB_DEV, dtype=jnp.int32)
    offset_step = jax.random.randint(key_step, (), 1, KB_DEV, dtype=jnp.int32)
    blocks = blocks.at[1].set((blocks[0] + offset_step) % KB_DEV)
    block_ids = owner_list * KB_DEV + blocks
    return block_ids[jax.random.permutation(key_order, NHOT)].astype(jnp.int32)


def draw_hot_blocks(key, part):
    return make_hot(key)


def draw_chosen_blocks(key, part):
    hot = make_hot(key)
    per_block = QB // KB
    count = KB_DEV + NHOT
    qblock = jnp.arange(NQB, dtype=jnp.int32)
    device = qblock // (TOK_DEV // QB)
    local_ids = device[:, None] * KB_DEV + jnp.arange(KB_DEV, dtype=jnp.int32)[None, :]
    candidates = jnp.concatenate([local_ids, jnp.broadcast_to(hot[None, :], (NQB, NHOT))], axis=1)
    noise = jax.random.randint(jax.random.fold_in(key, 7002), (NQB, count), 0, 1000, dtype=jnp.int32)
    first_own = qblock * per_block
    own_cover = (candidates >= first_own[:, None]) & (candidates < first_own[:, None] + per_block)
    earlier = candidates < first_own[:, None] + per_block
    duplicate = (jnp.arange(count, dtype=jnp.int32)[None, :] >= KB_DEV) & (candidates // KB_DEV == device[:, None])
    score = noise + 10000 * earlier.astype(jnp.int32) + 100000 * own_cover.astype(jnp.int32)
    score = score - 1000000 * duplicate.astype(jnp.int32)
    score = score * count + jnp.arange(count, dtype=jnp.int32)[None, :]
    _, picked = lax.top_k(score, NSEL)
    return picked.astype(jnp.int32)


def draw_head_scale(key, part):
    key_low = jax.random.fold_in(jax.random.fold_in(key, 7003), 1)
    return jnp.exp(jax.random.uniform(key_low, (H,), jnp.float32, math.log(0.5), math.log(4.0)))


def levels(own_key, shape, cuts, low, high):
    level, own = 1.0, jax.random.fold_in(own_key, 6)
    for axis_at, parts in cuts:
        heights = jnp.exp(jax.random.uniform(jax.random.fold_in(own, axis_at), (parts,), jnp.float32, low / len(cuts), high / len(cuts)))
        level = level * jnp.repeat(heights, shape[axis_at] // parts).reshape([-1 if axis == axis_at else 1 for axis in range(len(shape))])
    return level


def gaussian(own_key, extent, deviation, limit, pieces=(), held_as=jnp.bfloat16):
    array = jax.random.normal(own_key, extent, jnp.float32) * deviation
    if len(pieces) > 0:
        array = levels(own_key, extent, pieces, -0.22, 0.18) * array
    return jnp.clip(array, min=-limit, max=limit).astype(held_as)


def setup_inputs(seed: int = 0) -> dict:
    splits = jax.random.split(jax.random.key(seed), 9)
    return {
        "hidden_rows": gaussian(splits[0], (SEQ, D), 1.0, 6.0, ((0, 256),)),
        "proj_query": gaussian(splits[1], (D, H * HD), D ** -0.5, 0.125, ((1, 4),)),
        "proj_key": gaussian(splits[2], (D, KVH * HD), D ** -0.5, 0.125, ((1, 4),)),
        "proj_value": gaussian(splits[3], (D, KVH * HD), D ** -0.5, 0.125, ((1, 4),)),
        "proj_output": gaussian(splits[4], (H * HD, D), (H * HD) ** -0.5, 0.125, ((0, 4),)),
        "head_scale": draw_head_scale(jax.random.fold_in(splits[8], 71), 0),
        "hot_blocks": draw_hot_blocks(jax.random.fold_in(splits[8], 71), 0),
        "chosen_blocks": draw_chosen_blocks(jax.random.fold_in(splits[8], 71), 0),
    }


def reference(hidden_rows, proj_query, proj_key, proj_value, proj_output, head_scale, hot_blocks, chosen_blocks):
    group_size = H // KVH
    per_device = TOK_DEV // QB
    queries = jnp.dot(hidden_rows, proj_query, preferred_element_type=jnp.float32).astype(jnp.bfloat16)
    key_proj = jnp.dot(hidden_rows, proj_key, preferred_element_type=jnp.float32).astype(jnp.bfloat16)
    value_proj = jnp.dot(hidden_rows, proj_value, preferred_element_type=jnp.float32).astype(jnp.bfloat16)
    queries = queries.reshape(NQB, QB, KVH, group_size, HD)
    key_proj = key_proj.reshape(NKB, KB, KVH, HD)
    value_proj = value_proj.reshape(NKB, KB, KVH, HD)
    scale_grid = head_scale.reshape(KVH, group_size)

    def attend(block_index):
        codes = chosen_blocks[block_index]
        holder = (block_index // per_device).astype(jnp.int32)
        hot_index = jnp.clip(codes - KB_DEV, 0, NHOT - 1).astype(jnp.int32)
        picked = jnp.where(codes < KB_DEV, holder * KB_DEV + codes, hot_blocks[hot_index]).astype(jnp.int32)
        key_rows = key_proj[picked].reshape(NSEL * KB, KVH, HD).astype(jnp.float32)
        value_rows = value_proj[picked].reshape(NSEL * KB, KVH, HD).astype(jnp.float32)
        query_rows = queries[block_index].astype(jnp.float32)
        scores = jnp.einsum('qcgd,lcd->cgql', query_rows, key_rows) * (HD ** -0.5)
        scores = scores * scale_grid[:, :, None, None]
        query_pos = block_index * QB + jnp.arange(QB, dtype=jnp.int32)
        key_pos = (picked[:, None] * KB + jnp.arange(KB, dtype=jnp.int32)[None, :]).reshape(NSEL * KB)
        visible = key_pos[None, :] <= query_pos[:, None]
        scores = jnp.where(visible[None, None], scores, -jnp.inf)
        row_max = jnp.max(scores, axis=-1, keepdims=True)
        lifted = jnp.exp(scores - row_max)
        weights = lifted / jnp.sum(lifted, axis=-1, keepdims=True)
        weights = lax.optimization_barrier(weights.astype(jnp.bfloat16)).astype(jnp.float32)
        attended = jnp.einsum('cgql,lcd->qcgd', weights, value_rows)
        return attended.reshape(QB, H * HD).astype(jnp.bfloat16)

    heads_out = lax.map(attend, jnp.arange(NQB, dtype=jnp.int32)).reshape(NQB * QB, H * HD)
    width = H * HD // N_TP
    total = jnp.zeros((NQB * QB, D), jnp.float32)
    for group_index in range(N_TP):
        begin = group_index * width
        partial_value = jnp.dot(heads_out[:, begin:begin + width], proj_output[begin:begin + width],
                          preferred_element_type=jnp.float32)
        total = total + lax.optimization_barrier(partial_value.astype(jnp.bfloat16)).astype(jnp.float32)
    return total.astype(jnp.bfloat16)
```

```python
import functools

import jax
import jax.numpy as jnp
from jax import lax
from jax.experimental import pallas as pl
from jax.experimental.pallas import tpu as pltpu
from jax.sharding import Mesh
from jax.sharding import PartitionSpec as P

HD = 64
KB = 32
QB = 64
NSEL = 16
NHOT = 16
FAR = 1 << 30
F32 = jnp.float32
BF16 = jnp.bfloat16
MESH = pl.DeviceIdType.MESH


def outward(count):
    return sorted(range(1, count), key=lambda k: -min(k, count - k))


def row_order(row):
    return sorted(range(1, row), key=lambda k: -min(k, row - k))


def kernel(
    dims,
    x_hbm,
    wq_hbm,
    wk_hbm,
    wv_hbm,
    wo_hbm,
    scale_hbm,
    hot_hbm,
    codes_hbm,
    out_ref,
    x,
    wq,
    wkv,
    wo,
    scale,
    hot,
    codes,
    local_kv,
    kv_all,
    vk_all,
    q_even,
    q_odd,
    bias,
    give,
    got,
    part,
    around,
    scores,
    weights,
    opp,
    via,
    side,
    arrived,
    own,
    in_sem,
    hot_send,
    hot_recv,
    tp_send,
    tp_recv,
):
    nz, ny, nc, ntp = dims
    row = ny * nc
    z = lax.axis_index("z")
    r = lax.axis_index("y") * nc + lax.axis_index("c")
    s = lax.axis_index("tp")
    tokens, width = x.shape
    blocks = tokens // QB
    own_blocks = tokens // KB
    keys = kv_all.shape[0]
    base = (z * row + r) * tokens

    def in_row(k):
        t = lax.rem(r + k, row)
        return {"y": t // nc, "c": lax.rem(t, nc)}

    def in_z(k):
        return {"z": lax.rem(z + k, nz)}

    right = {"tp": lax.rem(s + 1, ntp)}
    left = {"tp": lax.rem(s + ntp - 1, ntp)}

    def load(i, src, dst):
        c = pltpu.make_async_copy(src, dst, in_sem.at[i])
        c.start()
        return c

    hot_in = load(0, hot_hbm, hot)
    kv_in = [load(1, x_hbm, x)]
    for i, src in enumerate((wk_hbm, wv_hbm, wv_hbm, wk_hbm)):
        kv_in.append(load(2 + i, src, wkv.at[pl.ds(HD * i, HD)]))
    q_in = load(6, wq_hbm, wq)
    codes_in = load(7, codes_hbm, codes)
    scale_in = load(8, scale_hbm, scale)
    wo_in = load(9, wo_hbm, wo)

    barrier = pltpu.get_barrier_semaphore()
    for k in outward(nz):
        pl.semaphore_signal(barrier, inc=1, device_id=in_z(k), device_id_type=MESH)
    for k in range(1, row):
        pl.semaphore_signal(barrier, inc=1, device_id=in_row(k), device_id_type=MESH)
    for peer in (left, right):
        pl.semaphore_signal(barrier, inc=1, device_id=peer, device_id_type=MESH)

    for c in kv_in:
        c.wait()
    both = lax.dot_general(
        x[...], wkv[...], (((1,), (1,)), ((), ())), preferred_element_type=F32
    ).astype(BF16)
    packed = both[:, : 2 * HD]
    local_kv[...] = packed.reshape(own_blocks, KB, 2 * HD)
    kv_all[pl.ds(0, tokens)] = packed
    vk_all[pl.ds(0, tokens)] = both[:, 2 * HD :]
    hot_in.wait()
    for j in range(NHOT):
        owner = hot[j] // own_blocks
        mine = owner == z * row + r
        block = local_kv[hot[j] - owner * own_blocks].astype(F32)
        give[j] = jnp.where(mine, block, 0.0).astype(BF16)

    pl.semaphore_wait(barrier, nz - 1 + row - 1 + 2)

    def first(k):
        return pltpu.make_async_remote_copy(
            give.at[lax.rem(r + k, row)], got.at[0, k], hot_send.at[0, k], hot_recv.at[0, k],
            device_id=in_row(k), device_id_type=MESH,
        )

    def second(k):
        return pltpu.make_async_remote_copy(
            part, got.at[1, k], hot_send.at[1, k], hot_recv.at[1, k],
            device_id=in_z(k), device_id_type=MESH,
        )

    def third(k):
        rows = pl.ds(pl.multiple_of(tokens + r * KB, KB), KB)
        return pltpu.make_async_remote_copy(
            around, kv_all.at[rows], hot_send.at[2, k], hot_recv.at[2, k],
            device_id=in_row(k), device_id_type=MESH,
        )

    for k in row_order(row):
        first(k).start()

    q_in.wait()
    pairs = wq.shape[1] // (2 * HD)
    low = lax.broadcasted_iota(jnp.int32, (QB, 2 * HD), 1) < HD
    queries = jnp.dot(x[...], wq[...], preferred_element_type=F32)
    for b in range(blocks):
        for i in range(pairs):
            tile = queries[b * QB : (b + 1) * QB, i * 2 * HD : (i + 1) * 2 * HD]
            q_even[b, pl.ds(i * QB, QB)] = jnp.where(low, tile, 0.0).astype(BF16)
            q_odd[b, pl.ds(i * QB, QB)] = jnp.where(low, 0.0, tile).astype(BF16)

    total = give[r].astype(F32)
    for k in range(1, row):
        first(k).wait_recv()
        total = total + got[0, k].astype(F32)
    part[...] = total.astype(BF16)
    for k in outward(nz):
        second(k).start()

    codes_in.wait()
    scale_in.wait()
    lane = lax.broadcasted_iota(jnp.int32, (8, keys), 1)
    number = lane >> 5
    key_pos = base + lane
    for j in range(NHOT):
        key_pos = jnp.where(number == own_blocks + j, hot[j] * KB + (lane & (KB - 1)), key_pos)
    for b in range(blocks):
        chosen = number == codes[b, 0]
        for e in range(1, NSEL):
            chosen = chosen | (number == codes[b, e])
        seen = jnp.where(chosen, key_pos, FAR)[0:1]
        query_pos = base + b * QB + lax.broadcasted_iota(jnp.int32, (QB, 1), 0)
        bias[b] = jnp.where(seen <= query_pos, 0.0, -jnp.inf)

    total = part[...].astype(F32)
    for k in range(1, nz):
        second(k).wait_recv()
        total = total + got[1, k].astype(F32)
    around[...] = total.astype(BF16)
    for k in row_order(row):
        third(k).start()
    kv_all[pl.ds(pl.multiple_of(tokens + r * KB, KB), KB)] = total.astype(BF16)
    wo_in.wait()
    for k in range(1, row):
        third(k).wait_recv()
    hot_rows = kv_all[pl.ds(tokens, NHOT * KB)].astype(F32)
    vk_all[pl.ds(tokens, NHOT * KB)] = pltpu.roll(hot_rows, HD, 1).astype(BF16)

    cols = wo.shape[1] // ntp
    half = cols // 2

    def copy(kind, c):
        src, dst, peer = (
            (opp.at[c, 0], via.at[c, 0], left),
            (opp.at[c, 1], via.at[c, 1], right),
            (side.at[c, 0, 1], arrived.at[c, 1, 1], left),
            (side.at[c, 1, 0], arrived.at[c, 0, 0], right),
            (side.at[c, 0, 0], arrived.at[c, 1, 0], left),
            (side.at[c, 1, 1], arrived.at[c, 0, 1], right),
        )[kind]
        return pltpu.make_async_remote_copy(
            src, dst, tp_send.at[kind, c], tp_recv.at[kind, c],
            device_id=peer, device_id_type=MESH,
        )

    def columns(shift):
        at = pl.multiple_of(lax.rem(s + shift, ntp) * cols, cols)
        return wo[:, pl.ds(at, cols)]

    def attend(b):
        outs = []
        for odd, q, rhs, val in ((0, q_even, kv_all, vk_all), (1, q_odd, vk_all, kv_all)):
            scores[odd] = lax.dot_general(
                q[b], rhs[...], (((1,), (1,)), ((), ())), preferred_element_type=F32
            )
            for i in range(pairs):
                factor = scale[2 * i + odd] * HD ** (-0.5)
                for p in range(2):
                    rows = pl.ds(i * QB + p * (QB // 2), QB // 2)
                    sc = scores[odd, rows] * factor + bias[b, pl.ds(p * (QB // 2), QB // 2)]
                    top = jnp.max(sc, axis=-1, keepdims=True)
                    lifted = jnp.exp(sc - top)
                    norm = 1.0 / jnp.sum(lifted, axis=-1, keepdims=True)
                    weights[odd, rows] = (lifted * norm).astype(BF16)
            outs.append(jnp.dot(weights[odd], val[...], preferred_element_type=F32))
        tiles = [
            jnp.where(low, outs[0][i * QB : (i + 1) * QB], outs[1][i * QB : (i + 1) * QB])
            for i in range(pairs)
        ]
        return jnp.concatenate(tiles, axis=1).astype(BF16)

    def produce(c):
        att = attend(c)
        far = jnp.dot(att, columns(2), preferred_element_type=F32).astype(BF16)
        opp[c, 0] = far[:, :half]
        opp[c, 1] = far[:, half:]
        copy(0, c).start()
        copy(1, c).start()
        to_left = jnp.dot(att, columns(ntp - 1), preferred_element_type=F32).astype(BF16)
        side[c, 0, 0] = to_left[:, :half]
        side[c, 0, 1] = to_left[:, half:]
        copy(2, c).start()
        to_right = jnp.dot(att, columns(1), preferred_element_type=F32).astype(BF16)
        side[c, 1, 0] = to_right[:, :half]
        side[c, 1, 1] = to_right[:, half:]
        copy(3, c).start()
        own[c] = jnp.dot(att, columns(0), preferred_element_type=F32).astype(BF16)

    def combine(c):
        for d in range(2):
            copy(d, c).wait_recv()
            side[c, d, d] = (side[c, d, d].astype(F32) + via[c, d].astype(F32)).astype(BF16)
            copy(4 + d, c).start()

    def finish(c):
        for kind in range(2, 6):
            copy(kind, c).wait_recv()
        rows = pl.ds(pl.multiple_of(c * QB, QB), QB)
        for h in range(2):
            part_sum = own[c, :, h * half : (h + 1) * half].astype(F32)
            part_sum = part_sum + arrived[c, 0, h].astype(F32) + arrived[c, 1, h].astype(F32)
            out_ref[rows, h * half : (h + 1) * half] = part_sum.astype(BF16)

    def step(c, carry):
        @pl.when(c < blocks)
        def _():
            produce(c)

        @pl.when((c >= 1) & (c <= blocks))
        def _():
            combine(c - 1)

        @pl.when(c >= 2)
        def _():
            finish(c - 2)

        return carry

    lax.fori_loop(0, blocks + 2, step, 0)

    for k in range(1, row):
        first(k).wait_send()
        third(k).wait_send()
    for k in range(1, nz):
        second(k).wait_send()
    for c in range(blocks):
        for kind in range(6):
            copy(kind, c).wait_send()


def local(
    dims,
    hidden_rows,
    proj_query,
    proj_key,
    proj_value,
    proj_output,
    head_scale,
    hot_blocks,
    chosen_blocks,
):
    nz, ny, nc, ntp = dims
    tokens, width = hidden_rows.shape
    head_cols = proj_query.shape[1]
    out_cols = proj_output.shape[1]
    cols = out_cols // ntp
    half = cols // 2
    blocks = tokens // QB
    keys = tokens + NHOT * KB
    stacked = head_cols // (2 * HD) * QB
    row = ny * nc
    anywhere = pl.BlockSpec(memory_space=pl.ANY)
    return pl.pallas_call(
        functools.partial(kernel, dims),
        out_shape=jax.ShapeDtypeStruct((tokens, cols), BF16),
        in_specs=[anywhere] * 8,
        out_specs=pl.BlockSpec(memory_space=pltpu.VMEM),
        scratch_shapes=[
            pltpu.VMEM((tokens, width), BF16),
            pltpu.VMEM((width, head_cols), BF16),
            pltpu.VMEM((4 * HD, width), BF16),
            pltpu.VMEM((head_cols, out_cols), BF16),
            pltpu.SMEM((head_cols // HD,), F32),
            pltpu.SMEM((NHOT,), jnp.int32),
            pltpu.SMEM((blocks, NSEL), jnp.int32),
            pltpu.VMEM((tokens // KB, KB, 2 * HD), BF16),
            pltpu.VMEM((keys, 2 * HD), BF16),
            pltpu.VMEM((keys, 2 * HD), BF16),
            pltpu.VMEM((blocks, stacked, 2 * HD), BF16),
            pltpu.VMEM((blocks, stacked, 2 * HD), BF16),
            pltpu.VMEM((blocks, QB, keys), F32),
            pltpu.VMEM((NHOT, KB, 2 * HD), BF16),
            pltpu.VMEM((2, NHOT, KB, 2 * HD), BF16),
            pltpu.VMEM((KB, 2 * HD), BF16),
            pltpu.VMEM((KB, 2 * HD), BF16),
            pltpu.VMEM((2, stacked, keys), F32),
            pltpu.VMEM((2, stacked, keys), BF16),
            pltpu.VMEM((blocks, 2, QB, half), BF16),
            pltpu.VMEM((blocks, 2, QB, half), BF16),
            pltpu.VMEM((blocks, 2, 2, QB, half), BF16),
            pltpu.VMEM((blocks, 2, 2, QB, half), BF16),
            pltpu.VMEM((blocks, QB, cols), BF16),
            pltpu.SemaphoreType.DMA((10,)),
            pltpu.SemaphoreType.DMA((3, NHOT)),
            pltpu.SemaphoreType.DMA((3, NHOT)),
            pltpu.SemaphoreType.DMA((6, blocks)),
            pltpu.SemaphoreType.DMA((6, blocks)),
        ],
        compiler_params=pltpu.CompilerParams(collective_id=0, has_side_effects=True),
    )(
        hidden_rows,
        proj_query,
        proj_key.T,
        proj_value.T,
        proj_output,
        head_scale,
        hot_blocks,
        chosen_blocks,
    )


def solution(mesh):
    ntp = mesh.shape["tp"]
    dims = (16, 8, 2, ntp)
    finer = Mesh(mesh.devices.reshape(dims), ("z", "y", "c", "tp"))
    kv = ("z", "y", "c")
    placed = (
        P(kv, None),
        P(None, "tp"),
        P(None, "tp"),
        P(None, "tp"),
        P("tp", None),
        P("tp"),
        P(),
        P(kv, None),
    )
    return jax.shard_map(
        functools.partial(local, dims),
        mesh=finer,
        in_specs=placed,
        out_specs=P(kv, "tp"),
        check_vma=False,
    )
```

```python
import functools

import jax
import jax.numpy as jnp
from jax import lax
from jax.experimental import pallas as pl
from jax.experimental.pallas import tpu as pltpu
from jax.sharding import Mesh
from jax.sharding import PartitionSpec as P

HD = 64
KB = 32
QB = 64
NSEL = 16
NHOT = 16
FAR = 1 << 30
PIECES = 4
LOG2E = 1.4426950408889634
F32 = jnp.float32
BF16 = jnp.bfloat16
MESH = pl.DeviceIdType.MESH


def row_order(row):
    return sorted(range(1, row), key=lambda k: -min(k, row - k))


def kernel(
    dims,
    x_hbm,
    wq_hbm,
    wk_hbm,
    wv_hbm,
    wo_hbm,
    scale_hbm,
    hot_hbm,
    codes_hbm,
    out_ref,
    x,
    wq,
    wkv,
    wo,
    scale,
    hot,
    codes,
    local_kv,
    kv_all,
    vk_all,
    q_even,
    q_odd,
    bias,
    give,
    got,
    part,
    around,
    scores,
    weights,
    local_out,
    local_top,
    local_sum,
    hot_sc,
    hot_w,
    attended,
    opp,
    via,
    side,
    arrived,
    own,
    in_sem,
    hot_send,
    hot_recv,
    tp_send,
    tp_recv,
    aware,
):
    nz, ny, nc, ntp = dims
    row = ny * nc
    z = lax.axis_index("z")
    r = lax.axis_index("y") * nc + lax.axis_index("c")
    s = lax.axis_index("tp")
    tokens, width = x.shape
    blocks = tokens // QB
    own_blocks = tokens // KB
    keys = kv_all.shape[0]
    base = (z * row + r) * tokens

    def in_row(k):
        t = lax.rem(r + k, row)
        return {"y": t // nc, "c": lax.rem(t, nc)}

    def in_z(k):
        return {"z": lax.rem(z + k, nz)}

    right = {"tp": lax.rem(s + 1, ntp)}
    left = {"tp": lax.rem(s + ntp - 1, ntp)}

    def load(i, src, dst):
        c = pltpu.make_async_copy(src, dst, in_sem.at[i])
        c.start()
        return c

    hot_in = load(0, hot_hbm, hot)
    kv_in = [
        load(1, wk_hbm, wkv.at[pl.ds(0, HD)]),
        load(2, wv_hbm, wkv.at[pl.ds(HD, HD)]),
    ]
    slab = width // PIECES
    slabs = [pl.ds(i * slab, slab) for i in range(PIECES)]
    x_in = [load(3 + i, x_hbm.at[:, at], x.at[:, at]) for i, at in enumerate(slabs)]

    barrier = pltpu.get_barrier_semaphore()
    for k in range(1, row):
        pl.semaphore_signal(barrier, inc=1, device_id=in_row(k), device_id_type=MESH)
    for peer in (left, right):
        pl.semaphore_signal(barrier, inc=1, device_id=peer, device_id_type=MESH)

    def above(d, carry):
        pl.semaphore_signal(barrier, inc=1, device_id={"z": d}, device_id_type=MESH)
        return carry

    lax.fori_loop(z + 1, nz, above, 0)

    for c in kv_in:
        c.wait()
    both = jnp.zeros((tokens, 2 * HD), F32)
    for c, at in zip(x_in, slabs):
        c.wait()
        both = both + lax.dot_general(
            x[:, at], wkv[:, at], (((1,), (1,)), ((), ())), preferred_element_type=F32
        )
    q_in = load(3 + PIECES, wq_hbm, wq)
    codes_in = load(4 + PIECES, codes_hbm, codes)
    scale_in = load(5 + PIECES, scale_hbm, scale)
    wo_in = load(6 + PIECES, wo_hbm, wo)
    packed = both.astype(BF16)
    local_kv[...] = packed.reshape(own_blocks, KB, 2 * HD)
    hot_in.wait()
    for j in range(NHOT):
        owner = hot[j] // own_blocks
        mine = owner == z * row + r
        block = local_kv[hot[j] - owner * own_blocks].astype(F32)
        give[j] = jnp.where(mine, block, 0.0).astype(BF16)

    pl.semaphore_wait(barrier, row - 1 + 2 + z)

    def first(k):
        return pltpu.make_async_remote_copy(
            give.at[lax.rem(r + k, row)], got.at[0, k], hot_send.at[0, k], hot_recv.at[0, k],
            device_id=in_row(k), device_id_type=MESH,
        )

    def second(k):
        return pltpu.make_async_remote_copy(
            part, got.at[1, k], hot_send.at[1, k], hot_recv.at[1, k],
            device_id=in_z(k), device_id_type=MESH,
        )

    def third(k):
        rows = pl.ds(pl.multiple_of(tokens + r * KB, KB), KB)
        return pltpu.make_async_remote_copy(
            around, kv_all.at[rows], hot_send.at[2, k], hot_recv.at[2, k],
            device_id=in_row(k), device_id_type=MESH,
        )

    def to_row(phase):
        for k in row_order(row):
            phase(k).start()

    to_row(first)

    def below(d, carry):
        pl.semaphore_signal(aware.at[z], inc=1, device_id={"z": d}, device_id_type=MESH)
        return carry

    lax.fori_loop(0, z, below, 0)
    kv_all[pl.ds(0, tokens)] = packed
    vk_all[pl.ds(0, tokens)] = pltpu.roll(packed.astype(F32), HD, 1).astype(BF16)

    q_in.wait()
    pairs = wq.shape[1] // (2 * HD)
    low = lax.broadcasted_iota(jnp.int32, (QB, 2 * HD), 1) < HD
    queries = jnp.dot(x[...], wq[...], preferred_element_type=F32)
    for b in range(blocks):
        for i in range(pairs):
            tile = queries[b * QB : (b + 1) * QB, i * 2 * HD : (i + 1) * 2 * HD]
            q_even[b, pl.ds(i * QB, QB)] = jnp.where(low, tile, 0.0).astype(BF16)
            q_odd[b, pl.ds(i * QB, QB)] = jnp.where(low, 0.0, tile).astype(BF16)

    total = give[r].astype(F32)
    for k in range(1, row):
        first(k).wait_recv()
        total = total + got[0, k].astype(F32)
    part[...] = total.astype(BF16)

    def sink(d, carry):
        second(lax.rem(d - z + nz, nz)).start()
        return carry

    lax.fori_loop(0, z, sink, 0)

    codes_in.wait()
    scale_in.wait()
    lane = lax.broadcasted_iota(jnp.int32, (8, keys), 1)
    number = lane >> 5
    key_pos = base + lane
    for j in range(NHOT):
        key_pos = jnp.where(number == own_blocks + j, hot[j] * KB + (lane & (KB - 1)), key_pos)
    for b in range(blocks):
        chosen = number == codes[b, 0]
        for e in range(1, NSEL):
            chosen = chosen | (number == codes[b, e])
        seen = jnp.where(chosen, key_pos, FAR)[0:1]
        query_pos = base + b * QB + lax.broadcasted_iota(jnp.int32, (QB, 1), 0)
        bias[b] = jnp.where(seen <= query_pos, 0.0, -jnp.inf)

    sides = ((0, q_even, kv_all, vk_all), (1, q_odd, vk_all, kv_all))
    quarter = QB // 2
    strips = [(i, p) for i in range(pairs) for p in range(2)]

    def scored(b, odd, q, rhs, first_key, count):
        at = pl.ds(first_key, count)
        scores[odd, :, pl.ds(0, count)] = lax.dot_general(
            q[b], rhs[at], (((1,), (1,)), ((), ())), preferred_element_type=F32
        )

    def strip(b, odd, i, p, first_key, count):
        rows = pl.ds(i * QB + p * quarter, quarter)
        factor = scale[2 * i + odd] * (HD ** (-0.5) * LOG2E)
        seen = bias[b, pl.ds(p * quarter, quarter), pl.ds(first_key, count)]
        return rows, scores[odd, rows, pl.ds(0, count)] * factor + seen

    def own_keys(b, carry):
        for odd, q, rhs, val in sides:
            scored(b, odd, q, rhs, 0, tokens)
            for i, p in strips:
                rows, sc = strip(b, odd, i, p, 0, tokens)
                top = jnp.max(sc, axis=-1, keepdims=True)
                lifted = jnp.exp2(sc - top)
                weights[odd, rows, pl.ds(0, tokens)] = lifted.astype(BF16)
                local_top[b, odd, rows] = top
                local_sum[b, odd, rows] = jnp.sum(lifted, axis=-1, keepdims=True)
            local_out[b, odd] = jnp.dot(
                weights[odd, :, pl.ds(0, tokens)], val[pl.ds(0, tokens)],
                preferred_element_type=F32,
            )
        return carry

    lax.fori_loop(0, blocks, own_keys, 0)

    def rise(d, carry):
        pl.semaphore_wait(aware.at[d], 1)
        second(d - z).start()
        return carry

    lax.fori_loop(z + 1, nz, rise, 0)

    total = part[...].astype(F32)
    for k in range(1, nz):
        second(k).wait_recv()
        total = total + got[1, k].astype(F32)
    around[...] = total.astype(BF16)
    to_row(third)
    kv_all[pl.ds(pl.multiple_of(tokens + r * KB, KB), KB)] = total.astype(BF16)
    wo_in.wait()
    for k in range(1, row):
        third(k).wait_recv()
    hot_rows = kv_all[pl.ds(tokens, NHOT * KB)].astype(F32)
    vk_all[pl.ds(tokens, NHOT * KB)] = pltpu.roll(hot_rows, HD, 1).astype(BF16)

    cols = wo.shape[1] // ntp
    half = cols // 2

    def copy(kind, c):
        src, dst, peer = (
            (opp.at[c, 0], via.at[c, 0], left),
            (opp.at[c, 1], via.at[c, 1], right),
            (side.at[c, 0, 1], arrived.at[c, 1, 1], left),
            (side.at[c, 1, 0], arrived.at[c, 0, 0], right),
            (side.at[c, 0, 0], arrived.at[c, 1, 0], left),
            (side.at[c, 1, 1], arrived.at[c, 0, 1], right),
        )[kind]
        return pltpu.make_async_remote_copy(
            src, dst, tp_send.at[kind, c], tp_recv.at[kind, c],
            device_id=peer, device_id_type=MESH,
        )

    def columns(shift):
        at = pl.multiple_of(lax.rem(s + shift, ntp) * cols, cols)
        return wo[:, pl.ds(at, cols)]

    count = NHOT * KB
    stacked = q_even.shape[1]

    def hot_scores(b):
        for odd, q, rhs, val in sides:
            both_q = q[pl.ds(b, 2)].reshape(2 * stacked, 2 * HD)
            hot_sc[odd] = lax.dot_general(
                both_q, rhs[pl.ds(tokens, count)], (((1,), (1,)), ((), ())),
                preferred_element_type=F32,
            )

    def attend(b, n):
        outs = []
        for odd, q, rhs, val in sides:
            kept, norms = [], []
            for i, p in strips:
                rows = pl.ds(i * QB + p * quarter, quarter)
                factor = scale[2 * i + odd] * (HD ** (-0.5) * LOG2E)
                seen = bias[b, pl.ds(p * quarter, quarter), pl.ds(tokens, count)]
                at = n * stacked + i * QB + p * quarter
                sc = hot_sc[odd, pl.ds(at, quarter)] * factor + seen
                before = local_top[b, odd, rows]
                top = jnp.maximum(before, jnp.max(sc, axis=-1, keepdims=True))
                lifted = jnp.exp2(sc - top)
                hot_w[n, odd, rows] = lifted.astype(BF16)
                fade = jnp.exp2(before - top)
                norm = 1.0 / (fade * local_sum[b, odd, rows] + jnp.sum(lifted, axis=-1, keepdims=True))
                kept.append(fade * norm)
                norms.append(norm)
            fresh = jnp.dot(
                hot_w[n, odd], val[pl.ds(tokens, count)], preferred_element_type=F32
            )
            tiles = []
            for m, (i, p) in enumerate(strips):
                at = i * QB + p * quarter
                tiles.append(
                    local_out[b, odd, pl.ds(at, quarter)] * kept[m]
                    + fresh[at : at + quarter] * norms[m]
                )
            outs.append(tiles)
        half_low = low[:quarter]
        heads = [
            jnp.concatenate(
                [jnp.where(half_low, outs[0][2 * i + p], outs[1][2 * i + p]) for p in range(2)],
                axis=0,
            )
            for i in range(pairs)
        ]
        return jnp.concatenate(heads, axis=1).astype(BF16)

    def combine(c, carry):
        for d in range(2):
            copy(d, c).wait_recv()
            side[c, d, d] = (side[c, d, d].astype(F32) + via[c, d].astype(F32)).astype(BF16)
            copy(4 + d, c).start()
        return carry

    def finish(c, carry):
        for kind in range(2, 6):
            copy(kind, c).wait_recv()
        for kind in range(6):
            copy(kind, c).wait_send()
        rows = pl.ds(pl.multiple_of(c * QB, QB), QB)
        for h in range(2):
            part_sum = own[c, :, h * half : (h + 1) * half].astype(F32)
            part_sum = part_sum + arrived[c, 0, h].astype(F32) + arrived[c, 1, h].astype(F32)
            out_ref[rows, h * half : (h + 1) * half] = part_sum.astype(BF16)
        return carry

    def product(att, shift):
        return jnp.dot(att, columns(shift), preferred_element_type=F32).astype(BF16)

    def produce(g, carry):
        hot_scores(2 * g)
        atts = []
        for n in range(2):
            c = 2 * g + n
            att = attend(c, n)
            atts.append(att)
            far = product(att, 2)
            opp[c, 0] = far[:, :half]
            opp[c, 1] = far[:, half:]
            copy(0, c).start()
            copy(1, c).start()
        att = jnp.concatenate(atts, axis=0)
        attended[pl.ds(pl.multiple_of(g * 2 * QB, 2 * QB), 2 * QB)] = att
        for d, shift in ((0, ntp - 1), (1, 1)):
            beside = product(att, shift)
            for n in range(2):
                part_rows = beside[n * QB : (n + 1) * QB]
                side[2 * g + n, d, 0] = part_rows[:, :half]
                side[2 * g + n, d, 1] = part_rows[:, half:]
                copy(2 + d, 2 * g + n).start()

        @pl.when(g > 0)
        def _():
            for n in range(2):
                combine(2 * g - 2 + n, 0)

        return carry

    lax.fori_loop(0, blocks // 2, produce, 0)
    own[...] = product(attended[...], 0).reshape(blocks, QB, cols)
    for n in range(2):
        combine(blocks - 2 + n, 0)
    for k in range(1, row):
        first(k).wait_send()
        third(k).wait_send()
    for k in range(1, nz):
        second(k).wait_send()
    lax.fori_loop(0, blocks, finish, 0)


def local(
    dims,
    hidden_rows,
    proj_query,
    proj_key,
    proj_value,
    proj_output,
    head_scale,
    hot_blocks,
    chosen_blocks,
):
    nz, ny, nc, ntp = dims
    tokens, width = hidden_rows.shape
    head_cols = proj_query.shape[1]
    out_cols = proj_output.shape[1]
    cols = out_cols // ntp
    half = cols // 2
    blocks = tokens // QB
    keys = tokens + NHOT * KB
    stacked = head_cols // (2 * HD) * QB
    row = ny * nc
    anywhere = pl.BlockSpec(memory_space=pl.ANY)
    return pl.pallas_call(
        functools.partial(kernel, dims),
        out_shape=pltpu.VMEM((tokens, cols), BF16),
        in_specs=[anywhere] * 8,
        out_specs=pl.BlockSpec(memory_space=pltpu.VMEM),
        scratch_shapes=[
            pltpu.VMEM((tokens, width), BF16),
            pltpu.VMEM((width, head_cols), BF16),
            pltpu.VMEM((2 * HD, width), BF16),
            pltpu.VMEM((head_cols, out_cols), BF16),
            pltpu.SMEM((head_cols // HD,), F32),
            pltpu.SMEM((NHOT,), jnp.int32),
            pltpu.SMEM((blocks, NSEL), jnp.int32),
            pltpu.VMEM((tokens // KB, KB, 2 * HD), BF16),
            pltpu.VMEM((keys, 2 * HD), BF16),
            pltpu.VMEM((keys, 2 * HD), BF16),
            pltpu.VMEM((blocks, stacked, 2 * HD), BF16),
            pltpu.VMEM((blocks, stacked, 2 * HD), BF16),
            pltpu.VMEM((blocks, QB, keys), F32),
            pltpu.VMEM((NHOT, KB, 2 * HD), BF16),
            pltpu.VMEM((2, NHOT, KB, 2 * HD), BF16),
            pltpu.VMEM((KB, 2 * HD), BF16),
            pltpu.VMEM((KB, 2 * HD), BF16),
            pltpu.VMEM((2, stacked, tokens), F32),
            pltpu.VMEM((2, stacked, tokens), BF16),
            pltpu.VMEM((blocks, 2, stacked, 2 * HD), F32),
            pltpu.VMEM((blocks, 2, stacked, 1), F32),
            pltpu.VMEM((blocks, 2, stacked, 1), F32),
            pltpu.VMEM((2, 2 * stacked, NHOT * KB), F32),
            pltpu.VMEM((2, 2, stacked, NHOT * KB), BF16),
            pltpu.VMEM((tokens, head_cols), BF16),
            pltpu.VMEM((blocks, 2, QB, half), BF16),
            pltpu.VMEM((blocks, 2, QB, half), BF16),
            pltpu.VMEM((blocks, 2, 2, QB, half), BF16),
            pltpu.VMEM((blocks, 2, 2, QB, half), BF16),
            pltpu.VMEM((blocks, QB, cols), BF16),
            pltpu.SemaphoreType.DMA((7 + PIECES,)),
            pltpu.SemaphoreType.DMA((3, NHOT)),
            pltpu.SemaphoreType.DMA((3, NHOT)),
            pltpu.SemaphoreType.DMA((6, blocks)),
            pltpu.SemaphoreType.DMA((6, blocks)),
            pltpu.SemaphoreType.REGULAR((16,)),
        ],
        compiler_params=pltpu.CompilerParams(collective_id=0, has_side_effects=True),
    )(
        hidden_rows,
        proj_query,
        proj_key.T,
        proj_value.T,
        proj_output,
        head_scale,
        hot_blocks,
        chosen_blocks,
    )


def solution(mesh):
    ntp = mesh.shape["tp"]
    dims = (16, 8, 2, ntp)
    finer = Mesh(mesh.devices.reshape(dims), ("z", "y", "c", "tp"))
    kv = ("z", "y", "c")
    placed = (
        P(kv, None),
        P(None, "tp"),
        P(None, "tp"),
        P(None, "tp"),
        P("tp", None),
        P("tp"),
        P(),
        P(kv, None),
    )
    return jax.shard_map(
        functools.partial(local, dims),
        mesh=finer,
        in_specs=placed,
        out_specs=P(kv, "tp"),
        check_vma=False,
    )
```

```python
import functools

import jax
import jax.numpy as jnp
from jax import lax
from jax.experimental import pallas as pl
from jax.experimental.pallas import tpu as pltpu
from jax.sharding import Mesh
from jax.sharding import PartitionSpec as P

HD = 64
KB = 32
QB = 64
NSEL = 16
NHOT = 16
FAR = 1 << 30
PIECES = 4
GROUP = 4
LOG2E = 1.4426950408889634
F32 = jnp.float32
BF16 = jnp.bfloat16
MESH = pl.DeviceIdType.MESH


def row_order(row):
    return sorted(range(1, row), key=lambda k: -min(k, row - k))


def kernel(
    dims,
    x_hbm,
    wq_hbm,
    wk_hbm,
    wv_hbm,
    wo_hbm,
    scale_hbm,
    hot_hbm,
    codes_hbm,
    out_ref,
    x,
    wq,
    wkv,
    wo,
    scale,
    hot,
    codes,
    local_kv,
    kv_all,
    vk_all,
    q_even,
    q_odd,
    bias,
    give,
    got,
    part,
    around,
    scores,
    weights,
    local_out,
    local_top,
    local_sum,
    hot_sc,
    hot_w,
    attended,
    opp,
    via,
    side,
    arrived,
    own,
    in_sem,
    hot_send,
    hot_recv,
    tp_send,
    tp_recv,
    aware,
):
    nz, ny, nc, ntp = dims
    row = ny * nc
    z = lax.axis_index("z")
    r = lax.axis_index("y") * nc + lax.axis_index("c")
    s = lax.axis_index("tp")
    tokens, width = x.shape
    blocks = tokens // QB
    own_blocks = tokens // KB
    keys = kv_all.shape[0]
    base = (z * row + r) * tokens

    def in_row(k):
        t = lax.rem(r + k, row)
        return {"y": t // nc, "c": lax.rem(t, nc)}

    def in_z(k):
        return {"z": lax.rem(z + k, nz)}

    right = {"tp": lax.rem(s + 1, ntp)}
    left = {"tp": lax.rem(s + ntp - 1, ntp)}

    def load(i, src, dst):
        c = pltpu.make_async_copy(src, dst, in_sem.at[i])
        c.start()
        return c

    hot_in = load(0, hot_hbm, hot)
    kv_in = [
        load(1, wk_hbm, wkv.at[pl.ds(0, HD)]),
        load(2, wv_hbm, wkv.at[pl.ds(HD, HD)]),
    ]
    slab = width // PIECES
    slabs = [pl.ds(i * slab, slab) for i in range(PIECES)]
    x_in = [load(3 + i, x_hbm.at[:, at], x.at[:, at]) for i, at in enumerate(slabs)]

    barrier = pltpu.get_barrier_semaphore()
    for k in range(1, row):
        pl.semaphore_signal(barrier, inc=1, device_id=in_row(k), device_id_type=MESH)
    for peer in (left, right):
        pl.semaphore_signal(barrier, inc=1, device_id=peer, device_id_type=MESH)

    def above(d, carry):
        pl.semaphore_signal(barrier, inc=1, device_id={"z": d}, device_id_type=MESH)
        return carry

    lax.fori_loop(z + 1, nz, above, 0)

    for c in kv_in:
        c.wait()
    both = jnp.zeros((tokens, 2 * HD), F32)
    for c, at in zip(x_in, slabs):
        c.wait()
        both = both + lax.dot_general(
            x[:, at], wkv[:, at], (((1,), (1,)), ((), ())), preferred_element_type=F32
        )
    q_in = load(3 + PIECES, wq_hbm, wq)
    codes_in = load(4 + PIECES, codes_hbm, codes)
    scale_in = load(5 + PIECES, scale_hbm, scale)
    wo_in = load(6 + PIECES, wo_hbm, wo)
    packed = both.astype(BF16)
    local_kv[...] = packed.reshape(own_blocks, KB, 2 * HD)
    hot_in.wait()
    for j in range(NHOT):
        owner = hot[j] // own_blocks
        mine = owner == z * row + r
        block = local_kv[hot[j] - owner * own_blocks].astype(F32)
        give[j] = jnp.where(mine, block, 0.0).astype(BF16)

    pl.semaphore_wait(barrier, row - 1 + 2 + z)

    def first(k):
        return pltpu.make_async_remote_copy(
            give.at[lax.rem(r + k, row)], got.at[0, k], hot_send.at[0, k], hot_recv.at[0, k],
            device_id=in_row(k), device_id_type=MESH,
        )

    def second(k):
        return pltpu.make_async_remote_copy(
            part, got.at[1, k], hot_send.at[1, k], hot_recv.at[1, k],
            device_id=in_z(k), device_id_type=MESH,
        )

    def passed(k):
        return pltpu.make_async_remote_copy(
            around, got.at[1, k], hot_send.at[1, k], hot_recv.at[1, k],
            device_id=in_z(k), device_id_type=MESH,
        )

    def third(k):
        rows = pl.ds(pl.multiple_of(tokens + r * KB, KB), KB)
        return pltpu.make_async_remote_copy(
            around, kv_all.at[rows], hot_send.at[2, k], hot_recv.at[2, k],
            device_id=in_row(k), device_id_type=MESH,
        )

    def to_row(phase):
        for k in row_order(row):
            phase(k).start()

    to_row(first)

    def below(d, carry):
        pl.semaphore_signal(aware.at[z], inc=1, device_id={"z": d}, device_id_type=MESH)
        return carry

    member = lax.rem(z, GROUP)

    @pl.when(member == 0)
    def _():
        lax.fori_loop(0, z, below, 0)

    @pl.when(member > 0)
    def _():
        below(z - member, 0)
    kv_all[pl.ds(0, tokens)] = packed
    vk_all[pl.ds(0, tokens)] = pltpu.roll(packed.astype(F32), HD, 1).astype(BF16)

    q_in.wait()
    pairs = wq.shape[1] // (2 * HD)
    low = lax.broadcasted_iota(jnp.int32, (QB, 2 * HD), 1) < HD
    queries = jnp.dot(x[...], wq[...], preferred_element_type=F32)
    for b in range(blocks):
        for i in range(pairs):
            tile = queries[b * QB : (b + 1) * QB, i * 2 * HD : (i + 1) * 2 * HD]
            q_even[b, pl.ds(i * QB, QB)] = jnp.where(low, tile, 0.0).astype(BF16)
            q_odd[b, pl.ds(i * QB, QB)] = jnp.where(low, 0.0, tile).astype(BF16)

    total = give[r].astype(F32)
    for k in range(1, row):
        first(k).wait_recv()
        total = total + got[0, k].astype(F32)
    part[...] = total.astype(BF16)

    def sink(g, carry):
        second(lax.rem(g * GROUP - z + nz, nz)).start()
        return carry

    lax.fori_loop(0, (z + GROUP - 1) // GROUP, sink, 0)

    codes_in.wait()
    scale_in.wait()
    lane = lax.broadcasted_iota(jnp.int32, (8, keys), 1)
    number = lane >> 5
    key_pos = base + lane
    for j in range(NHOT):
        key_pos = jnp.where(number == own_blocks + j, hot[j] * KB + (lane & (KB - 1)), key_pos)
    for b in range(blocks):
        chosen = number == codes[b, 0]
        for e in range(1, NSEL):
            chosen = chosen | (number == codes[b, e])
        seen = jnp.where(chosen, key_pos, FAR)[0:1]
        query_pos = base + b * QB + lax.broadcasted_iota(jnp.int32, (QB, 1), 0)
        bias[b] = jnp.where(seen <= query_pos, 0.0, -jnp.inf)

    sides = ((0, q_even, kv_all, vk_all), (1, q_odd, vk_all, kv_all))
    quarter = QB // 2
    strips = [(i, p) for i in range(pairs) for p in range(2)]

    def scored(b, odd, q, rhs, first_key, count):
        at = pl.ds(first_key, count)
        scores[odd, :, pl.ds(0, count)] = lax.dot_general(
            q[b], rhs[at], (((1,), (1,)), ((), ())), preferred_element_type=F32
        )

    def strip(b, odd, i, p, first_key, count):
        rows = pl.ds(i * QB + p * quarter, quarter)
        factor = scale[2 * i + odd] * (HD ** (-0.5) * LOG2E)
        seen = bias[b, pl.ds(p * quarter, quarter), pl.ds(first_key, count)]
        return rows, scores[odd, rows, pl.ds(0, count)] * factor + seen

    def own_keys(b, carry):
        for odd, q, rhs, val in sides:
            scored(b, odd, q, rhs, 0, tokens)
            for i, p in strips:
                rows, sc = strip(b, odd, i, p, 0, tokens)
                top = jnp.max(sc, axis=-1, keepdims=True)
                lifted = jnp.exp2(sc - top)
                weights[odd, rows, pl.ds(0, tokens)] = lifted.astype(BF16)
                local_top[b, odd, rows] = top
                local_sum[b, odd, rows] = jnp.sum(lifted, axis=-1, keepdims=True)
            local_out[b, odd] = jnp.dot(
                weights[odd, :, pl.ds(0, tokens)], val[pl.ds(0, tokens)],
                preferred_element_type=F32,
            )
        return carry

    lax.fori_loop(0, blocks, own_keys, 0)

    def rise(g, carry):
        pl.semaphore_wait(aware.at[g * GROUP], 1)
        second(g * GROUP - z).start()
        return carry

    lax.fori_loop(z // GROUP + 1, nz // GROUP, rise, 0)

    @pl.when(member == 0)
    def _():
        whole = part[...].astype(F32)
        for k in range(1, nz):
            second(k).wait_recv()
            whole = whole + got[1, k].astype(F32)
        around[...] = whole.astype(BF16)
        for k in range(1, GROUP):
            pl.semaphore_wait(aware.at[z + k], 1)
            passed(k).start()

    @pl.when(member > 0)
    def _():
        passed(member).wait_recv()
        around[...] = got[1, member]

    to_row(third)
    kv_all[pl.ds(pl.multiple_of(tokens + r * KB, KB), KB)] = around[...]
    wo_in.wait()
    for k in range(1, row):
        third(k).wait_recv()
    hot_rows = kv_all[pl.ds(tokens, NHOT * KB)].astype(F32)
    vk_all[pl.ds(tokens, NHOT * KB)] = pltpu.roll(hot_rows, HD, 1).astype(BF16)

    cols = wo.shape[1] // ntp
    half = cols // 2

    def copy(kind, c):
        src, dst, peer = (
            (opp.at[c, 0], via.at[c, 0], left),
            (opp.at[c, 1], via.at[c, 1], right),
            (side.at[c, 0, 1], arrived.at[c, 1, 1], left),
            (side.at[c, 1, 0], arrived.at[c, 0, 0], right),
            (side.at[c, 0, 0], arrived.at[c, 1, 0], left),
            (side.at[c, 1, 1], arrived.at[c, 0, 1], right),
        )[kind]
        return pltpu.make_async_remote_copy(
            src, dst, tp_send.at[kind, c], tp_recv.at[kind, c],
            device_id=peer, device_id_type=MESH,
        )

    def columns(shift):
        at = pl.multiple_of(lax.rem(s + shift, ntp) * cols, cols)
        return wo[:, pl.ds(at, cols)]

    count = NHOT * KB
    stacked = q_even.shape[1]

    def hot_scores(b):
        for odd, q, rhs, val in sides:
            both_q = q[pl.ds(b, 2)].reshape(2 * stacked, 2 * HD)
            hot_sc[odd] = lax.dot_general(
                both_q, rhs[pl.ds(tokens, count)], (((1,), (1,)), ((), ())),
                preferred_element_type=F32,
            )

    def attend(b, n):
        outs = []
        for odd, q, rhs, val in sides:
            kept, norms = [], []
            for i, p in strips:
                rows = pl.ds(i * QB + p * quarter, quarter)
                factor = scale[2 * i + odd] * (HD ** (-0.5) * LOG2E)
                seen = bias[b, pl.ds(p * quarter, quarter), pl.ds(tokens, count)]
                at = n * stacked + i * QB + p * quarter
                sc = hot_sc[odd, pl.ds(at, quarter)] * factor + seen
                before = local_top[b, odd, rows]
                top = jnp.maximum(before, jnp.max(sc, axis=-1, keepdims=True))
                lifted = jnp.exp2(sc - top)
                hot_w[n, odd, rows] = lifted.astype(BF16)
                fade = jnp.exp2(before - top)
                norm = 1.0 / (fade * local_sum[b, odd, rows] + jnp.sum(lifted, axis=-1, keepdims=True))
                kept.append(fade * norm)
                norms.append(norm)
            fresh = jnp.dot(
                hot_w[n, odd], val[pl.ds(tokens, count)], preferred_element_type=F32
            )
            tiles = []
            for m, (i, p) in enumerate(strips):
                at = i * QB + p * quarter
                tiles.append(
                    local_out[b, odd, pl.ds(at, quarter)] * kept[m]
                    + fresh[at : at + quarter] * norms[m]
                )
            outs.append(tiles)
        half_low = low[:quarter]
        heads = [
            jnp.concatenate(
                [jnp.where(half_low, outs[0][2 * i + p], outs[1][2 * i + p]) for p in range(2)],
                axis=0,
            )
            for i in range(pairs)
        ]
        return jnp.concatenate(heads, axis=1).astype(BF16)

    def combine(c, carry):
        for d in range(2):
            copy(d, c).wait_recv()
            side[c, d, d] = (side[c, d, d].astype(F32) + via[c, d].astype(F32)).astype(BF16)
            copy(4 + d, c).start()
        return carry

    def finish(c, carry):
        for kind in range(2, 6):
            copy(kind, c).wait_recv()
        for kind in range(6):
            copy(kind, c).wait_send()
        rows = pl.ds(pl.multiple_of(c * QB, QB), QB)
        for h in range(2):
            part_sum = own[c, :, h * half : (h + 1) * half].astype(F32)
            part_sum = part_sum + arrived[c, 0, h].astype(F32) + arrived[c, 1, h].astype(F32)
            out_ref[rows, h * half : (h + 1) * half] = part_sum.astype(BF16)
        return carry

    def product(att, shift):
        return jnp.dot(att, columns(shift), preferred_element_type=F32).astype(BF16)

    def produce(g, carry):
        hot_scores(2 * g)
        atts = []
        for n in range(2):
            c = 2 * g + n
            att = attend(c, n)
            atts.append(att)
            far = product(att, 2)
            opp[c, 0] = far[:, :half]
            opp[c, 1] = far[:, half:]
            copy(0, c).start()
            copy(1, c).start()
        att = jnp.concatenate(atts, axis=0)
        attended[pl.ds(pl.multiple_of(g * 2 * QB, 2 * QB), 2 * QB)] = att
        for d, shift in ((0, ntp - 1), (1, 1)):
            beside = product(att, shift)
            for n in range(2):
                part_rows = beside[n * QB : (n + 1) * QB]
                side[2 * g + n, d, 0] = part_rows[:, :half]
                side[2 * g + n, d, 1] = part_rows[:, half:]
                copy(2 + d, 2 * g + n).start()

        @pl.when(g > 0)
        def _():
            for n in range(2):
                combine(2 * g - 2 + n, 0)

        return carry

    lax.fori_loop(0, blocks // 2, produce, 0)
    own[...] = product(attended[...], 0).reshape(blocks, QB, cols)
    for n in range(2):
        combine(blocks - 2 + n, 0)
    for k in range(1, row):
        first(k).wait_send()
        third(k).wait_send()
    for g in range(nz // GROUP):

        @pl.when(g * GROUP != z)
        def _():
            second(lax.rem(g * GROUP - z + nz, nz)).wait_send()

    @pl.when(member == 0)
    def _():
        for k in range(1, GROUP):
            passed(k).wait_send()

    lax.fori_loop(0, blocks, finish, 0)


def local(
    dims,
    hidden_rows,
    proj_query,
    proj_key,
    proj_value,
    proj_output,
    head_scale,
    hot_blocks,
    chosen_blocks,
):
    nz, ny, nc, ntp = dims
    tokens, width = hidden_rows.shape
    head_cols = proj_query.shape[1]
    out_cols = proj_output.shape[1]
    cols = out_cols // ntp
    half = cols // 2
    blocks = tokens // QB
    keys = tokens + NHOT * KB
    stacked = head_cols // (2 * HD) * QB
    row = ny * nc
    anywhere = pl.BlockSpec(memory_space=pl.ANY)
    return pl.pallas_call(
        functools.partial(kernel, dims),
        out_shape=pltpu.VMEM((tokens, cols), BF16),
        in_specs=[anywhere] * 8,
        out_specs=pl.BlockSpec(memory_space=pltpu.VMEM),
        scratch_shapes=[
            pltpu.VMEM((tokens, width), BF16),
            pltpu.VMEM((width, head_cols), BF16),
            pltpu.VMEM((2 * HD, width), BF16),
            pltpu.VMEM((head_cols, out_cols), BF16),
            pltpu.SMEM((head_cols // HD,), F32),
            pltpu.SMEM((NHOT,), jnp.int32),
            pltpu.SMEM((blocks, NSEL), jnp.int32),
            pltpu.VMEM((tokens // KB, KB, 2 * HD), BF16),
            pltpu.VMEM((keys, 2 * HD), BF16),
            pltpu.VMEM((keys, 2 * HD), BF16),
            pltpu.VMEM((blocks, stacked, 2 * HD), BF16),
            pltpu.VMEM((blocks, stacked, 2 * HD), BF16),
            pltpu.VMEM((blocks, QB, keys), F32),
            pltpu.VMEM((NHOT, KB, 2 * HD), BF16),
            pltpu.VMEM((2, NHOT, KB, 2 * HD), BF16),
            pltpu.VMEM((KB, 2 * HD), BF16),
            pltpu.VMEM((KB, 2 * HD), BF16),
            pltpu.VMEM((2, stacked, tokens), F32),
            pltpu.VMEM((2, stacked, tokens), BF16),
            pltpu.VMEM((blocks, 2, stacked, 2 * HD), F32),
            pltpu.VMEM((blocks, 2, stacked, 1), F32),
            pltpu.VMEM((blocks, 2, stacked, 1), F32),
            pltpu.VMEM((2, 2 * stacked, NHOT * KB), F32),
            pltpu.VMEM((2, 2, stacked, NHOT * KB), BF16),
            pltpu.VMEM((tokens, head_cols), BF16),
            pltpu.VMEM((blocks, 2, QB, half), BF16),
            pltpu.VMEM((blocks, 2, QB, half), BF16),
            pltpu.VMEM((blocks, 2, 2, QB, half), BF16),
            pltpu.VMEM((blocks, 2, 2, QB, half), BF16),
            pltpu.VMEM((blocks, QB, cols), BF16),
            pltpu.SemaphoreType.DMA((7 + PIECES,)),
            pltpu.SemaphoreType.DMA((3, NHOT)),
            pltpu.SemaphoreType.DMA((3, NHOT)),
            pltpu.SemaphoreType.DMA((6, blocks)),
            pltpu.SemaphoreType.DMA((6, blocks)),
            pltpu.SemaphoreType.REGULAR((16,)),
        ],
        compiler_params=pltpu.CompilerParams(collective_id=0, has_side_effects=True),
    )(
        hidden_rows,
        proj_query,
        proj_key.T,
        proj_value.T,
        proj_output,
        head_scale,
        hot_blocks,
        chosen_blocks,
    )


def solution(mesh):
    ntp = mesh.shape["tp"]
    dims = (16, 8, 2, ntp)
    finer = Mesh(mesh.devices.reshape(dims), ("z", "y", "c", "tp"))
    kv = ("z", "y", "c")
    placed = (
        P(kv, None),
        P(None, "tp"),
        P(None, "tp"),
        P(None, "tp"),
        P("tp", None),
        P("tp"),
        P(),
        P(kv, None),
    )
    return jax.shard_map(
        functools.partial(local, dims),
        mesh=finer,
        in_specs=placed,
        out_specs=P(kv, "tp"),
        check_vma=False,
    )
```
